32 devices in a mesh: sp: 8 (over z, x), tp: 4 (over y, core).
Axes of the slice: x: 2, y: 2, z: 4, core: 2. Of those that a mesh axis runs over, the one named last changes fastest.
Arguments:
- sequence_activations: bfloat16 [4096, 2048], P('sp', 'tp'), may hold values from -45 to 45
- entry_rescale_vector: float32 [2048], replicated, may hold values from 0.1 to 1.9
- blender_exit_switch_matrix: bfloat16 [2048, 2048], P('sp', 'tp'), may hold values from -0.125 to 0.125
- blender_entry_switch_matrix: bfloat16 [2048, 2048], P('sp', 'tp'), may hold values from -0.125 to 0.125
- blender_payload_matrix: bfloat16 [2048, 2048], P('sp', 'tp'), may hold values from -0.125 to 0.125
- scan_entry_matrix: bfloat16 [2048, 2048], P('sp', 'tp'), may hold values from -0.125 to 0.125
- scan_exit_switch_matrix: bfloat16 [2048, 2048], P('sp', 'tp'), may hold values from -0.125 to 0.125
- filter_blend_matrix: bfloat16 [2048, 2048], P('sp', 'tp'), may hold values from -0.125 to 0.125
- scan_blend_matrix: bfloat16 [2048, 2048], P('sp', 'tp'), may hold values from -0.125 to 0.125
- blender_kernel_coefficients: bfloat16 [3, 2048], P(None, 'tp'), may hold values from -3.5 to 3.5
- scan_kernel_coefficients: bfloat16 [4, 2048], P(None, 'tp'), may hold values from -3 to 3
- scan_switch_blockwise: bfloat16 [8, 256, 256], P('tp'), may hold values from -0.375 to 0.375
- entry_switch_blockwise: bfloat16 [8, 256, 256], P('tp'), may hold values from -0.375 to 0.375
- feature_fade_odds: float32 [2048], P('tp'), may hold values from 3 to 16
- fade_speed_multiplier: float32 [4096], P('sp'), may hold values from 0.3 to 2.8
- added_rate_shift: float32 [4096], P('sp'), may hold values from -1.4 to 0
- initial_hidden_vector: float32 [2048], P('tp'), may hold values from -6 to 6
- filter_exit_matrix: bfloat16 [2048, 2048], P('tp'), may hold values from -0.125 to 0.125
- scan_exit_matrix: bfloat16 [2048, 2048], P('tp'), may hold values from -0.125 to 0.125
Outputs:
- mixed: bfloat16 [4096, 2048], P('sp', 'tp')
The draws below stay inside these ranges and needn't reach their ends.
All inputs are finite; a program needn't handle non-finite values.
Results may differ from the reference program's by a relative error of at most 0.015.
Values may be sent and summed in bfloat16 or wider, within the bound.
A program may use at most 64 MiB of HBM per device.

```python
import jax
import jax.numpy as jnp
from jax import lax

D = 2048
CONV_WIDTH = 2048
LRU_WIDTH = 2048
LRU_HEADS = 8
HEAD_DIM = 256
SHORT_K = 3
LRU_K = 4
TOK_DEV = 512
SEQ = 4096
N_TP = 4


def draw_sequence_activations(key, part):
    key_base, key_rows = jax.random.split(key)
    base = jnp.clip(jax.random.normal(key_base, (SEQ, D), jnp.float32), -5.0, 5.0)
    rise = 3.0
    columns = rise ** (jnp.arange(D, dtype=jnp.float32) / (D - 1))
    row_scale = jnp.exp(jax.random.uniform(key_rows, (SEQ, 1), jnp.float32, jnp.log(0.3), jnp.log(3.0)))
    return (base * columns[None, :] * row_scale / rise ** 0.5).astype(jnp.bfloat16)


def draw_feature_fade_odds(key, part):
    key_pick, key_fast, key_slow = jax.random.split(key, 3)
    share = 0.5
    fast_mask = jax.random.uniform(key_pick, (LRU_WIDTH,), jnp.float32) < share
    fast_rate = jnp.exp(jax.random.uniform(key_fast, (LRU_WIDTH,), jnp.float32, jnp.log(0.01), jnp.log(0.033))) / 4.0
    slow_rate = jnp.exp(jax.random.uniform(key_slow, (LRU_WIDTH,), jnp.float32, jnp.log(0.1), jnp.log(0.4))) / (4.0 * SEQ)
    rate = jnp.where(fast_mask, fast_rate, slow_rate)
    return (-rate - jnp.log(-jnp.expm1(-rate))).astype(jnp.float32)


def draw_fade_speed_multiplier(key, part):
    key_block, key_rough = jax.random.split(key)
    block_count = SEQ // TOK_DEV
    block_scale = jnp.exp(jax.random.uniform(key_block, (block_count,), jnp.float32, jnp.log(0.5), jnp.log(2.0)))
    rough = jax.random.uniform(key_rough, (SEQ,), jnp.float32, 0.6, 1.4)
    return (jnp.repeat(block_scale, TOK_DEV) * rough).astype(jnp.float32)


def draw_added_rate_shift(key, part):
    key_place, key_depth = jax.random.split(key)
    places = jax.random.randint(key_place, (2,), 0, SEQ)
    depth = jax.random.uniform(key_depth, (2,), jnp.float32, jnp.log(0.5), jnp.log(0.8))
    position = jnp.arange(SEQ)
    first_hit = jnp.where(position == places[0], depth[0], 0.0)
    second_hit = jnp.where(position == places[1], depth[1], 0.0)
    return (first_hit + second_hit).astype(jnp.float32)


def level_of(key, shape, pieces, low, largest):
    gain = 1.0
    for axis_at, blocks in pieces:
        heights = jax.random.uniform(jax.random.fold_in(jax.random.fold_in(key, 6), axis_at), (blocks,), jnp.float32, low / len(pieces), largest / len(pieces))
        gain = gain * jnp.repeat(jnp.exp(heights), shape[axis_at] // blocks).reshape((-1,) + (1,) * (len(shape) - 1 - axis_at))
    return gain


def centred(key, extent, scale, most, cuts=(), kind=jnp.bfloat16):
    array = jax.random.normal(key, extent, jnp.float32) * scale
    if len(cuts) > 0:
        array = level_of(key, extent, cuts, -0.22, 0.18) * array
    return jnp.clip(array, min=-most, max=most).astype(kind)


def setup_inputs(seed: int = 0) -> dict:
    streams_of = jax.random.split(jax.random.key(seed), 20)
    sequence_activations = draw_sequence_activations(jax.random.fold_in(streams_of[19], 71), 0)
    entry_rescale_vector = jnp.clip(1.0 + 0.18 * jax.random.normal(streams_of[1], (D,), jnp.float32), 0.1, 1.9)
    blender_exit_switch_matrix = centred(streams_of[2], (D, CONV_WIDTH), D ** -0.5, 0.125, ((0, 8), (1, 4)))
    blender_entry_switch_matrix = centred(streams_of[3], (D, CONV_WIDTH), D ** -0.5, 0.125, ((0, 8), (1, 4)))
    blender_payload_matrix = centred(streams_of[4], (D, CONV_WIDTH), D ** -0.5, 0.125, ((0, 8), (1, 4)))
    scan_entry_matrix = centred(streams_of[5], (D, LRU_WIDTH), D ** -0.5, 0.125, ((0, 8), (1, 4)))
    scan_exit_switch_matrix = centred(streams_of[6], (D, LRU_WIDTH), D ** -0.5, 0.125, ((0, 8), (1, 4)))
    filter_blend_matrix = centred(streams_of[7], (D, D), D ** -0.5, 0.125, ((0, 8), (1, 4)))
    scan_blend_matrix = centred(streams_of[8], (D, D), D ** -0.5, 0.125, ((0, 8), (1, 4)))
    blender_kernel_coefficients = centred(streams_of[9], (SHORT_K, CONV_WIDTH), SHORT_K ** -0.5, 3.5, ((1, 4),))
    scan_kernel_coefficients = centred(streams_of[10], (LRU_K, LRU_WIDTH), LRU_K ** -0.5, 3.0, ((1, 4),))
    scan_switch_blockwise = centred(streams_of[11], (LRU_HEADS, HEAD_DIM, HEAD_DIM), HEAD_DIM ** -0.5, 0.375, ((0, 4),))
    entry_switch_blockwise = centred(streams_of[12], (LRU_HEADS, HEAD_DIM, HEAD_DIM), HEAD_DIM ** -0.5, 0.375, ((0, 4),))
    feature_fade_odds = draw_feature_fade_odds(jax.random.fold_in(streams_of[19], 71), 0)
    fade_speed_multiplier = draw_fade_speed_multiplier(jax.random.fold_in(streams_of[19], 71), 0)
    added_rate_shift = draw_added_rate_shift(jax.random.fold_in(streams_of[19], 71), 0)
    initial_hidden_vector = centred(streams_of[16], (LRU_WIDTH,), 1.0, 6.0, ((0, 4),), jnp.float32)
    filter_exit_matrix = centred(streams_of[17], (CONV_WIDTH, D), CONV_WIDTH ** -0.5, 0.125, ((0, 4),))
    scan_exit_matrix = centred(streams_of[18], (LRU_WIDTH, D), LRU_WIDTH ** -0.5, 0.125, ((0, 4),))
    return dict(sequence_activations=sequence_activations, entry_rescale_vector=entry_rescale_vector, blender_exit_switch_matrix=blender_exit_switch_matrix, blender_entry_switch_matrix=blender_entry_switch_matrix, blender_payload_matrix=blender_payload_matrix, scan_entry_matrix=scan_entry_matrix, scan_exit_switch_matrix=scan_exit_switch_matrix, filter_blend_matrix=filter_blend_matrix, scan_blend_matrix=scan_blend_matrix, blender_kernel_coefficients=blender_kernel_coefficients, scan_kernel_coefficients=scan_kernel_coefficients, scan_switch_blockwise=scan_switch_blockwise, entry_switch_blockwise=entry_switch_blockwise, feature_fade_odds=feature_fade_odds, fade_speed_multiplier=fade_speed_multiplier, added_rate_shift=added_rate_shift, initial_hidden_vector=initial_hidden_vector, filter_exit_matrix=filter_exit_matrix, scan_exit_matrix=scan_exit_matrix)


scan_switch_exponent = 8.0
norm_eps = 1e-06

def causal_taps(values, weights):
    taps = weights.shape[0]
    length = values.shape[0]
    padded = jnp.pad(values, ((taps - 1, 0), (0, 0)))
    result = padded[0:length] * weights[0].astype(jnp.float32)
    for tap_index in range(1, taps):
        result = result + padded[tap_index:tap_index + length] * weights[tap_index].astype(jnp.float32)
    return result

def linear_chain(earlier, later):
    return (earlier[0] * later[0], later[0] * earlier[1] + later[1])

def rounded_partials(branch_in, weight):
    width = branch_in.shape[1] // N_TP
    total = jnp.zeros((branch_in.shape[0], weight.shape[1]), jnp.float32)
    for block in range(N_TP):
        partial_sum = jnp.dot(branch_in[:, block * width:(block + 1) * width], weight[block * width:(block + 1) * width], preferred_element_type=jnp.float32).astype(jnp.bfloat16)
        total = total + lax.optimization_barrier(partial_sum).astype(jnp.float32)
    return total

def reference(sequence_activations, entry_rescale_vector, blender_exit_switch_matrix, blender_entry_switch_matrix, blender_payload_matrix, scan_entry_matrix, scan_exit_switch_matrix, filter_blend_matrix, scan_blend_matrix, blender_kernel_coefficients, scan_kernel_coefficients, scan_switch_blockwise, entry_switch_blockwise, feature_fade_odds, fade_speed_multiplier, added_rate_shift, initial_hidden_vector, filter_exit_matrix, scan_exit_matrix):
    token_float = sequence_activations.astype(jnp.float32)
    inverse = lax.rsqrt(lax.optimization_barrier(jnp.mean(token_float * token_float, axis=1, keepdims=True)) + norm_eps)
    scaled = (token_float * entry_rescale_vector).astype(jnp.bfloat16)

    def project(weight):
        return (jnp.dot(scaled, weight, preferred_element_type=jnp.float32) * inverse).astype(jnp.bfloat16)
    conv_b = project(blender_exit_switch_matrix)
    conv_c = project(blender_entry_switch_matrix)
    conv_x = project(blender_payload_matrix)
    lru_in = project(scan_entry_matrix)
    lru_gate = project(scan_exit_switch_matrix)
    mix_conv = project(filter_blend_matrix)
    mix_lru = project(scan_blend_matrix)
    short_in = conv_c.astype(jnp.float32) * conv_x.astype(jnp.float32)
    conv_mix = (conv_b.astype(jnp.float32) * causal_taps(short_in, blender_kernel_coefficients)).astype(jnp.bfloat16)
    lru_conv = causal_taps(lru_in.astype(jnp.float32), scan_kernel_coefficients).astype(jnp.bfloat16)
    length = sequence_activations.shape[0]
    heads = lru_conv.astype(jnp.float32).reshape(length, LRU_HEADS, HEAD_DIM)
    scan_switch_amount = jax.nn.sigmoid(jnp.einsum('thi,hij->thj', heads, scan_switch_blockwise.astype(jnp.float32))).reshape(length, LRU_WIDTH)
    gate_i = jax.nn.sigmoid(jnp.einsum('thi,hij->thj', heads, entry_switch_blockwise.astype(jnp.float32))).reshape(length, LRU_WIDTH)
    fade_exponent_multiplier = scan_switch_exponent * scan_switch_amount * jax.nn.log_sigmoid(feature_fade_odds)[None, :] * fade_speed_multiplier[:, None] + added_rate_shift[:, None]
    decay = jnp.exp(fade_exponent_multiplier)
    scale = jnp.sqrt(-jnp.expm1(2.0 * fade_exponent_multiplier))
    first = (jnp.arange(length) == 0)[:, None]
    scale = jnp.where(first, jnp.float32(1.0), scale)
    drive = scale * gate_i * lru_conv.astype(jnp.float32)
    decay_blocks = decay.reshape(length // TOK_DEV, TOK_DEV, LRU_WIDTH)
    drive_blocks = drive.reshape(length // TOK_DEV, TOK_DEV, LRU_WIDTH)

    def block_step(carry, block):
        cum_decay, cum_drive = lax.associative_scan(linear_chain, block, axis=0)
        states = cum_drive + cum_decay * carry[None, :]
        return (states[-1], states)
    start_state = initial_hidden_vector.astype(jnp.float32)
    last_state, states = lax.scan(block_step, start_state, (decay_blocks, drive_blocks))
    state = states.reshape(length, LRU_WIDTH)
    lru_mix = (state * jax.nn.gelu(lru_gate.astype(jnp.float32), approximate=True)).astype(jnp.bfloat16)
    conv_sum = rounded_partials(conv_mix, filter_exit_matrix)
    lru_sum = rounded_partials(lru_mix, scan_exit_matrix)
    mixed = jax.nn.sigmoid(mix_conv.astype(jnp.float32)) * conv_sum + jax.nn.sigmoid(mix_lru.astype(jnp.float32)) * lru_sum
    return mixed.astype(jnp.bfloat16)
```

```python
import functools

import jax
import jax.numpy as jnp
from jax import lax
from jax.experimental import pallas as pl
from jax.experimental.pallas import tpu as pltpu
from jax.sharding import PartitionSpec as P

scan_switch_exponent = 8.0
norm_eps = 1e-06


def passed_along(value, axis, by):
    peers = lax.axis_size(axis)
    pairs = [(i, i + by) for i in range(peers) if 0 <= i + by < peers]
    return lax.ppermute(value, axis, pairs)


def entering(value, axis, combine, identity):
    peers, place = (lax.axis_size(axis), lax.axis_index(axis))
    everything = jax.tree.map(lambda part: lax.all_gather(part, axis), value)
    start = jax.tree.map(
        lambda part, zero: jnp.broadcast_to(jnp.asarray(zero, part.dtype), part.shape),
        value,
        identity,
    )

    def step(k, before):
        reached = k < place
        new = combine(before, jax.tree.map(lambda part: part[k], everything))
        return jax.tree.map(lambda a, b: jnp.where(reached, a, b), new, before)

    return lax.fori_loop(0, peers, step, start)


def linear_chain(earlier, later):
    return (earlier[0] * later[0], later[0] * earlier[1] + later[1])


def causal_local(previous, values, weights):
    taps = weights.shape[0]
    length = values.shape[0]
    extended = jnp.concatenate([previous, values], axis=0)
    result = extended[0:length] * weights[0].astype(jnp.float32)
    for tap_index in range(1, taps):
        result = result + extended[tap_index : tap_index + length] * weights[tap_index].astype(
            jnp.float32
        )
    return result


def local(
    sequence_activations,
    entry_rescale_vector,
    blender_exit_switch_matrix,
    blender_entry_switch_matrix,
    blender_payload_matrix,
    scan_entry_matrix,
    scan_exit_switch_matrix,
    filter_blend_matrix,
    scan_blend_matrix,
    blender_kernel_coefficients,
    scan_kernel_coefficients,
    scan_switch_blockwise,
    entry_switch_blockwise,
    feature_fade_odds,
    fade_speed_multiplier,
    added_rate_shift,
    initial_hidden_vector,
    filter_exit_matrix,
    scan_exit_matrix,
):
    row_count = sequence_activations.shape[0]
    feature_count = entry_rescale_vector.shape[0]
    pieces = [
        blender_exit_switch_matrix,
        blender_entry_switch_matrix,
        blender_payload_matrix,
        scan_entry_matrix,
        scan_exit_switch_matrix,
        filter_blend_matrix,
        scan_blend_matrix,
    ]
    local_cat = jnp.concatenate(pieces, axis=1)
    whole_weight = lax.all_gather(local_cat, "sp", axis=0, tiled=True)
    piece = lax.all_gather(sequence_activations, "tp", axis=1, tiled=True)
    piece_float = piece.astype(jnp.float32)
    scaled_piece = (piece.astype(jnp.float32) * entry_rescale_vector[None, :]).astype(jnp.bfloat16)
    totals = jnp.dot(scaled_piece, whole_weight, preferred_element_type=jnp.float32)
    squares = jnp.sum(piece_float * piece_float, axis=1)
    inverse = lax.rsqrt(squares / feature_count + norm_eps)
    projected = (totals * inverse[:, None]).astype(jnp.bfloat16)
    outputs = []
    offset = 0
    for weight in pieces:
        outputs.append(projected[:, offset : offset + weight.shape[1]])
        offset = offset + weight.shape[1]
    conv_b, conv_c, conv_x, lru_in, lru_gate, mix_conv, mix_lru = outputs
    short_in = conv_c.astype(jnp.float32) * conv_x.astype(jnp.float32)
    lru_float = lru_in.astype(jnp.float32)
    short_edge = blender_kernel_coefficients.shape[0] - 1
    lru_edge = scan_kernel_coefficients.shape[0] - 1
    prev_short, prev_lru = passed_along(
        (short_in[row_count - short_edge :], lru_float[row_count - lru_edge :]), "sp", 1
    )
    lru_conv = causal_local(prev_lru, lru_float, scan_kernel_coefficients).astype(jnp.bfloat16)
    head_local = scan_switch_blockwise.shape[0]
    head_size = scan_switch_blockwise.shape[1]
    lru_local = lru_conv.shape[1]
    heads = lru_conv.reshape(row_count, head_local, head_size)
    scan_switch_amount = jax.nn.sigmoid(
        jnp.einsum("thi,hij->thj", heads, scan_switch_blockwise, preferred_element_type=jnp.float32)
    ).reshape(row_count, lru_local)
    gate_i = jax.nn.sigmoid(
        jnp.einsum(
            "thi,hij->thj", heads, entry_switch_blockwise, preferred_element_type=jnp.float32
        )
    ).reshape(row_count, lru_local)
    position = lax.axis_index("sp") * row_count + jnp.arange(row_count, dtype=jnp.int32)
    fade_exponent_multiplier = (
        scan_switch_exponent
        * scan_switch_amount
        * jax.nn.log_sigmoid(feature_fade_odds)[None, :]
        * fade_speed_multiplier[:, None]
        + added_rate_shift[:, None]
    )
    decay = jnp.exp(fade_exponent_multiplier)
    scale = jnp.sqrt(-jnp.expm1(2.0 * fade_exponent_multiplier))
    scale = jnp.where((position == 0)[:, None], jnp.float32(1.0), scale)
    drive = scale * gate_i * lru_conv.astype(jnp.float32)
    cum_decay, cum_drive = lax.associative_scan(linear_chain, (decay, drive), axis=0)
    ones_state = jnp.ones((lru_local,), jnp.float32)
    zero_state = jnp.zeros((lru_local,), jnp.float32)
    pref_decay, pref_state = entering(
        (cum_decay[-1], cum_drive[-1]), "sp", linear_chain, (ones_state, zero_state)
    )
    carry_in = pref_decay * initial_hidden_vector + pref_state
    state = cum_drive + cum_decay * carry_in[None, :]
    lru_mix = (state * jax.nn.gelu(lru_gate.astype(jnp.float32), approximate=True)).astype(
        jnp.bfloat16
    )
    conv_mix = (
        conv_b.astype(jnp.float32) * causal_local(prev_short, short_in, blender_kernel_coefficients)
    ).astype(jnp.bfloat16)
    conv_part = jnp.dot(conv_mix, filter_exit_matrix, preferred_element_type=jnp.float32)
    lru_part = jnp.dot(lru_mix, scan_exit_matrix, preferred_element_type=jnp.float32)
    conv_sum, lru_sum = (
        lax.psum_scatter(
            conv_part.astype(jnp.bfloat16), "tp", scatter_dimension=1, tiled=True
        ).astype(jnp.float32),
        lax.psum_scatter(
            lru_part.astype(jnp.bfloat16), "tp", scatter_dimension=1, tiled=True
        ).astype(jnp.float32),
    )
    mixed = (
        jax.nn.sigmoid(mix_conv.astype(jnp.float32)) * conv_sum
        + jax.nn.sigmoid(mix_lru.astype(jnp.float32)) * lru_sum
    )
    return mixed.astype(jnp.bfloat16)


MESH = pl.DeviceIdType.MESH
F32, BF16 = jnp.float32, jnp.bfloat16


def small_log1p(u):
    w = 1.0 + u
    return jnp.where(w == 1.0, u, jnp.log(w) * u / jnp.where(w == 1.0, 1.0, w - 1.0))


def neg_expm1(v):
    near = 1.0 + v * (1.0 / 8.0)
    for n in (7, 6, 5, 4, 3, 2):
        near = 1.0 + v * (1.0 / n) * near
    return jnp.where(v > -0.5, -v * near, 1.0 - jnp.exp(v))


def fused_kernel(
    sizes,
    x_hbm, gain, w0, w1, w2, w3, w4, w5, w6,
    ctaps, ltaps, wr, wi, odds, pos, init, ec_hbm, el_hbm,
    out,
    wbuf, xg, xs, sq, inv, posn, lbuf, abuf, bbuf, cbuf, carry_in, carry_out, sbuf,
    mix, got, parts, rbuf, sums, ebuf,
    wl, wx_s, wx_r, zr_s, zr_r, zl_s, zl_r, xg_s, xg_r, po_s, po_r, ed_s, ed_r,
    xe_s, xe_r, rs_s, rs_r, loc,
):
    sp, tp = sizes
    nz = sp // 2
    s, t = lax.axis_index("sp"), lax.axis_index("tp")
    z, x = s // 2, lax.rem(s, 2)
    xo = 1 - x
    half = wbuf.shape[3]
    rows = x_hbm.shape[0]
    krows = w0.shape[0]
    feats = x_hbm.shape[1]
    both = 2 * rows
    tile = half
    segs = 8
    seg = both // segs
    weights = (w0, w1, w2, w3, w4, w5, w6)
    count = len(weights)
    xn = (s + 1 - 2 * x, t)
    core = t + 1 - 2 * lax.rem(t, 2)
    ty = lax.rem(t + 2, tp)
    tyc = lax.rem(core + 2, tp)
    has_l, has_r = z > 0, z < nz - 1
    left, right = (s - 2, t), (s + 2, t)

    def remote(src, dst, ss, rs, dev):
        return pltpu.make_async_remote_copy(
            src_ref=src, dst_ref=dst, send_sem=ss, recv_sem=rs, device_id=dev, device_id_type=MESH
        )

    bar = pltpu.get_barrier_semaphore()
    pl.semaphore_signal(bar, inc=1, device_id=xn, device_id_type=MESH)
    for j in range(1, tp):
        pl.semaphore_signal(bar, inc=1, device_id=(s, lax.rem(t + j, tp)), device_id_type=MESH)

    @pl.when(has_l)
    def _():
        pl.semaphore_signal(bar, inc=1, device_id=left, device_id_type=MESH)

    @pl.when(has_r)
    def _():
        pl.semaphore_signal(bar, inc=1, device_id=right, device_id_type=MESH)

    own_cols = pl.ds(pl.multiple_of(x * half, half), half)
    other_cols = pl.ds(pl.multiple_of(xo * half, half), half)

    def own_half(p):
        return pltpu.make_async_copy(
            weights[p].at[:, own_cols], wbuf.at[p, z, x], wl.at[p]
        )

    def swap_half(p):
        return remote(weights[p].at[:, other_cols], wbuf.at[p, z, x], wx_s.at[p], wx_r.at[p], xn)

    def swap_half_in(p):
        return remote(weights[p].at[:, other_cols], wbuf.at[p, z, xo], wx_s.at[p], wx_r.at[p], xn)

    x_in = pltpu.make_async_copy(x_hbm, xg.at[x, t], loc.at[2])
    exits = (
        pltpu.make_async_copy(el_hbm, ebuf.at[0], loc.at[0]),
        pltpu.make_async_copy(ec_hbm, ebuf.at[1], loc.at[1]),
    )
    x_in.start()
    for p in range(count):
        own_half(p).start()
    pl.semaphore_wait(bar, tp + jnp.where(has_l, 1, 0) + jnp.where(has_r, 1, 0))

    swap_half(0).start()
    x_moves = {
        0: lambda: remote(x_hbm, xg.at[x, t], xg_s.at[0], xg_r.at[0], xn),
        1: lambda: remote(x_hbm, xg.at[x, t], xg_s.at[1], xg_r.at[1], (s, ty)),
        2: lambda: remote(x_hbm, xg.at[x, t], xg_s.at[2], xg_r.at[2], (s, core)),
        3: lambda: remote(xg.at[xo, t], xg.at[xo, t], xg_s.at[3], xg_r.at[3], (s, ty)),
        4: lambda: remote(xg.at[xo, t], xg.at[xo, t], xg_s.at[4], xg_r.at[4], (s, core)),
        5: lambda: remote(xg.at[x, ty], xg.at[x, ty], xg_s.at[5], xg_r.at[5], (s, core)),
        6: lambda: remote(xg.at[xo, ty], xg.at[xo, ty], xg_s.at[6], xg_r.at[6], (s, core)),
    }
    x_slots = {
        0: (xo, t), 1: (x, ty), 2: (x, core), 3: (xo, ty),
        4: (xo, core), 5: (x, tyc), 6: (xo, tyc),
    }

    def x_arrive(k):
        a, b = x_slots[k]
        remote(xg.at[a, b], xg.at[a, b], xg_s.at[k], xg_r.at[k], (s, core)).wait_recv()

    for k in (0, 1, 2):
        x_moves[k]().start()
    pos_out = remote(pos, posn.at[x], po_s, po_r, xn)
    pos_out.start()
    for p in range(1, count):
        swap_half(p).start()
    for e in exits:
        e.start()

    def z_right(p, d):
        ref = wbuf.at[p, z - d]
        return remote(ref, ref, zr_s.at[p, d], zr_r.at[p, d], right)

    def z_left(p, d):
        ref = wbuf.at[p, z + d]
        return remote(ref, ref, zl_s.at[p, d], zl_r.at[p, d], left)

    def from_left(p, d):
        ref = wbuf.at[p, z - 1 - d]
        return remote(ref, ref, zr_s.at[p, d], zr_r.at[p, d], right)

    def from_right(p, d):
        ref = wbuf.at[p, z + 1 + d]
        return remote(ref, ref, zl_s.at[p, d], zl_r.at[p, d], left)

    def issue_own(p):
        if p >= count:
            return
        own_half(p).wait()
        swap_half_in(p).wait_recv()

        @pl.when(has_r)
        def _():
            z_right(p, 0).start()

        @pl.when(has_l)
        def _():
            z_left(p, 0).start()

    relayed = set()

    def relay(p, d):
        if p >= count or d >= nz - 1 or (p, d) in relayed:
            return
        relayed.add((p, d))

        @pl.when(z - 1 - d >= 0)
        def _():
            from_left(p, d).wait_recv()
            if d + 1 < nz - 1:
                @pl.when(has_r)
                def _():
                    z_right(p, d + 1).start()

        @pl.when(z + 1 + d < nz)
        def _():
            from_right(p, d).wait_recv()
            if d + 1 < nz - 1:
                @pl.when(has_l)
                def _():
                    z_left(p, d + 1).start()

    def scale_block(a, b):
        for i in range(rows // tile):
            piece = xg[a, b, pl.ds(i * tile, tile), :].astype(F32)
            at = pl.ds(pl.multiple_of(a * rows + i * tile, tile), tile)
            xs[b, at, :] = (piece * gain[b]).astype(BF16)
            square = piece * piece
            total = square[:, 0:128]
            for c in range(1, feats // 128):
                total = total + square[:, c * 128 : (c + 1) * 128]
            sq[at, :] += total

    issue_own(0)
    issue_own(1)
    sq[...] = jnp.zeros_like(sq)
    x_in.wait()
    scale_block(x, t)
    relay(0, 0)
    issue_own(2)
    x_arrive(2)
    scale_block(x, core)
    x_arrive(0)
    x_moves[3]().start()
    x_moves[4]().start()
    x_arrive(1)
    x_moves[5]().start()
    relay(0, 1)
    scale_block(xo, t)
    scale_block(x, ty)
    x_arrive(3)
    x_moves[6]().start()
    relay(0, 2)
    scale_block(xo, ty)
    x_arrive(4)
    scale_block(xo, core)
    x_arrive(5)
    scale_block(x, tyc)
    relay(1, 0)
    x_arrive(6)
    scale_block(xo, tyc)
    total = jnp.sum(sq[...], axis=1, keepdims=True)
    inv[...] = jnp.broadcast_to(lax.rsqrt(total / (feats * tp) + norm_eps), inv.shape)
    posn[x] = pos[...]
    remote(pos, posn.at[xo], po_s, po_r, xn).wait_recv()

    def project(p, use):
        per = krows * 2

        def step(i, _):
            at = pl.ds(pl.multiple_of(i * tile, tile), tile)
            acc = None
            for b in range(tp):
                lhs = xs[b, at, :]
                for zz in range(b * feats // per, (b + 1) * feats // per):
                    for xx in range(2):
                        k0 = zz * per + xx * krows - b * feats
                        term = jnp.dot(
                            lhs[:, k0 : k0 + krows], wbuf[p, zz, xx], preferred_element_type=F32
                        )
                        acc = term if acc is None else acc + term
            wide = inv[at, :]
            scale = jnp.concatenate([wide] * (half // 128), axis=1)
            use(at, i, (acc * scale).astype(BF16))
            return 0

        lax.fori_loop(0, both // tile, step, 0)

    def edge(buf, k):
        return remote(buf.at[pl.ds(both, 8)], buf.at[pl.ds(0, 8)], ed_s.at[k], ed_r.at[k], right)

    def edge_send(buf, k):
        @pl.when(has_r)
        def _():
            edge(buf, k).start()

        @pl.when(z == 0)
        def _():
            buf[0:8, :] = jnp.zeros((8, half), F32)

    def edge_wait(buf, k):
        @pl.when(has_l)
        def _():
            edge(buf, k).wait_recv()

    def carry_copy():
        return remote(carry_out, carry_in, ed_s.at[2], ed_r.at[2], right)

    def swap(k):
        at = pl.ds(pl.multiple_of(xo * rows, rows), rows)
        return remote(mix.at[k, at], got.at[k, x], xe_s.at[k], xe_r.at[k], xn)

    def swap_start(k):
        swap(k).start()
        at = pl.ds(pl.multiple_of(x * rows, rows), rows)
        got[k, x] = mix[k, at, :]

    def swap_wait(k):
        remote(mix.at[k, pl.ds(0, rows)], got.at[k, xo], xe_s.at[k], xe_r.at[k], xn).wait_recv()

    def exchange(e, j):
        peer = lax.rem(t + j, tp)
        return remote(parts.at[e, j], rbuf.at[e, j], rs_s.at[e, j], rs_r.at[e, j], (s, peer))

    def exit_matmul(e):
        exits[e].wait()
        for j in list(range(1, tp)) + [0]:
            peer = lax.rem(t + j, tp)
            cols = pl.ds(pl.multiple_of(peer * feats, feats), feats)

            def step(i, _):
                at = pl.ds(pl.multiple_of(i * tile, tile), tile)
                acc = jnp.dot(
                    got[e, 0, at, :], ebuf[e, 0:half, cols], preferred_element_type=F32
                ) + jnp.dot(
                    got[e, 1, at, :], ebuf[e, half : 2 * half, cols], preferred_element_type=F32
                )
                parts[e, j, at, :] = acc.astype(BF16)
                return 0

            lax.fori_loop(0, rows // tile, step, 0)
            if j > 0:
                exchange(e, j).start()

    def exit_sum(e):
        for j in range(1, tp):
            exchange(e, j).wait_recv()
        total = parts[e, 0].astype(F32)
        for j in range(1, tp):
            total = total + rbuf[e, j].astype(F32)
        sums[e] = total

    def finish_stage(p):
        for d in range(nz - 1):
            relay(p, d)
        issue_own(p + 3)

    issue_own(3)

    def keep_lru(at, i, value):
        lbuf[pl.ds(pl.multiple_of(8 + i * tile, 8), tile), :] = value.astype(F32)

    project(0, keep_lru)
    edge_send(lbuf, 0)
    relay(1, 1)
    edge_wait(lbuf, 0)
    rate = -scan_switch_exponent * small_log1p(jnp.exp(-odds[:, own_cols]))
    lanes = ltaps[:, own_cols].astype(F32)
    taps = ltaps.shape[0]
    for i in range(both // tile):
        conv = None
        for k in range(taps):
            term = lbuf[pl.ds(8 - (taps - 1) + k + i * tile, tile), :] * lanes[k : k + 1]
            conv = term if conv is None else conv + term
        conv = conv.astype(BF16)
        gate_r = jax.nn.sigmoid(jnp.dot(conv, wr[x], preferred_element_type=F32))
        gate_i = jax.nn.sigmoid(jnp.dot(conv, wi[x], preferred_element_type=F32))
        first = (i * tile) // rows
        local_at = i * tile - first * rows
        turned = posn[first].T
        speed = turned[local_at : local_at + tile, 0:1]
        shift = turned[local_at : local_at + tile, 1:2]
        log_a = gate_r * rate * speed + shift
        gain_in = jnp.sqrt(neg_expm1(2.0 * log_a))
        if i == 0:
            row = lax.broadcasted_iota(jnp.int32, gain_in.shape, 0) + z * both
            gain_in = jnp.where(row == 0, 1.0, gain_in)
        decay = jnp.exp(log_a)
        drive = gain_in * gate_i * conv.astype(F32)
        for c in range(half // 128):
            cols = slice(c * 128, (c + 1) * 128)
            abuf[c, pl.ds(i * tile, tile), :] = decay[:, cols]
            bbuf[c, pl.ds(i * tile, tile), :] = drive[:, cols]

    lanes_n = half // 128

    def scan_step(i, held):
        cum, state = list(held[:lanes_n]), list(held[lanes_n:])
        at = pl.ds(i, segs, stride=seg)
        for c in range(lanes_n):
            a = abuf[c, at, :]
            state[c] = a * state[c] + bbuf[c, at, :]
            cum[c] = cum[c] * a
            abuf[c, at, :] = cum[c]
            bbuf[c, at, :] = state[c]
        return tuple(cum) + tuple(state)

    ends = lax.fori_loop(
        0, seg, scan_step,
        tuple(jnp.ones((segs, 128), F32) for _ in range(lanes_n))
        + tuple(jnp.zeros((segs, 128), F32) for _ in range(lanes_n)),
        unroll=8,
    )
    end_a = jnp.concatenate(ends[:lanes_n], axis=1)
    end_b = jnp.concatenate(ends[lanes_n:], axis=1)

    @pl.when(z == 0)
    def _():
        carry_in[...] = jnp.broadcast_to(init[:, own_cols], carry_in.shape)

    finish_stage(1)

    @pl.when(has_l)
    def _():
        carry_copy().wait_recv()

    carry = carry_in[0:1, :]
    for j in range(segs):
        cbuf[j : j + 1, :] = carry
        carry = end_b[j : j + 1] + end_a[j : j + 1] * carry
    carry_out[...] = jnp.broadcast_to(carry, carry_out.shape)

    @pl.when(has_r)
    def _():
        carry_copy().start()

    def keep_gate(at, i, value):
        gate = jax.nn.gelu(value.astype(F32), approximate=True)
        pieces = []
        for j in range(tile // seg):
            here = pl.ds(pl.multiple_of(i * tile + j * seg, seg), seg)
            c = cbuf[pl.ds(i * (tile // seg) + j, 1), :]
            pieces.append(
                jnp.concatenate(
                    [
                        bbuf[n, here, :] + abuf[n, here, :] * c[:, n * 128 : (n + 1) * 128]
                        for n in range(half // 128)
                    ],
                    axis=1,
                )
            )
        mix[0, at, :] = (jnp.concatenate(pieces, axis=0) * gate).astype(BF16)

    project(1, keep_gate)
    swap_start(0)
    finish_stage(2)

    def keep_c(at, i, value):
        sbuf[pl.ds(pl.multiple_of(8 + i * tile, 8), tile), :] = value.astype(F32)

    project(2, keep_c)
    swap_wait(0)
    exit_matmul(0)
    finish_stage(3)

    def keep_cx(at, i, value):
        here = pl.ds(pl.multiple_of(8 + i * tile, 8), tile)
        sbuf[here, :] = sbuf[here, :] * value.astype(F32)

    project(3, keep_cx)
    edge_send(sbuf, 1)
    finish_stage(4)

    def keep_b(at, i, value):
        lbuf[pl.ds(pl.multiple_of(8 + i * tile, 8), tile), :] = value.astype(F32)

    @pl.when(has_r)
    def _():
        edge(lbuf, 0).wait_send()

    project(4, keep_b)
    edge_wait(sbuf, 1)
    clanes = ctaps[:, own_cols].astype(F32)
    ktaps = ctaps.shape[0]
    for i in range(both // tile):
        conv = None
        for k in range(ktaps):
            term = sbuf[pl.ds(8 - (ktaps - 1) + k + i * tile, tile), :] * clanes[k : k + 1]
            conv = term if conv is None else conv + term
        mix[1, pl.ds(i * tile, tile), :] = (lbuf[pl.ds(8 + i * tile, tile), :] * conv).astype(BF16)
    swap_start(1)
    relay(5, 0)
    relay(5, 1)
    swap_wait(1)
    exit_matmul(1)
    for d in range(2, nz - 1):
        relay(5, d)

    def keep_mix(k):
        def use(at, i, value):
            mix[k, at, :] = value
        return use

    project(5, keep_mix(2))
    swap_start(2)
    exit_sum(0)
    for d in range(nz - 1):
        relay(6, d)
    project(6, keep_mix(3))
    swap_start(3)
    exit_sum(1)
    swap_wait(2)
    swap_wait(3)
    for xx in range(2):
        cols = slice(xx * half, (xx + 1) * half)
        out[:, cols] = (
            jax.nn.sigmoid(got[2, xx].astype(F32)) * sums[1, :, cols]
            + jax.nn.sigmoid(got[3, xx].astype(F32)) * sums[0, :, cols]
        ).astype(BF16)

    pos_out.wait_send()
    for p in range(count):
        swap_half(p).wait_send()
        for d in range(nz - 1):
            @pl.when(has_r & (z - d >= 0))
            def _():
                z_right(p, d).wait_send()

            @pl.when(has_l & (z + d < nz))
            def _():
                z_left(p, d).wait_send()
    for k in x_moves:
        x_moves[k]().wait_send()

    @pl.when(has_r)
    def _():
        edge(sbuf, 1).wait_send()
        carry_copy().wait_send()

    for k in range(4):
        swap(k).wait_send()
    for e in range(2):
        for j in range(1, tp):
            exchange(e, j).wait_send()


def paired(sizes, *args):
    (
        x, gain, wb, wc, wx, win, wgate, mconv, mlru, ctaps, ltaps, wr, wi,
        odds, speed, shift, init, ec, el,
    ) = args
    sp, tp = sizes
    nz = sp // 2
    rows, feats = x.shape
    krows, width = wb.shape
    half = width // 2
    both = 2 * rows
    pos = jnp.concatenate(
        [speed[None], shift[None], jnp.zeros((6, rows), F32)], axis=0
    )
    vmem = pl.BlockSpec(memory_space=pltpu.VMEM)
    anys = pl.BlockSpec(memory_space=pl.ANY)
    dma = pltpu.SemaphoreType.DMA
    kernel = pl.pallas_call(
        functools.partial(fused_kernel, sizes),
        out_shape=jax.ShapeDtypeStruct((rows, width), BF16),
        in_specs=[anys, vmem] + [anys] * 7 + [vmem] * 7 + [anys] * 2,
        out_specs=vmem,
        scratch_shapes=[
            pltpu.VMEM((7, nz, 2, krows, half), BF16),
            pltpu.VMEM((2, tp, rows, feats), BF16),
            pltpu.VMEM((tp, both, feats), BF16),
            pltpu.VMEM((both, 128), F32),
            pltpu.VMEM((both, 128), F32),
            pltpu.VMEM((2, 8, rows), F32),
            pltpu.VMEM((both + 8, half), F32),
            pltpu.VMEM((half // 128, both, 128), F32),
            pltpu.VMEM((half // 128, both, 128), F32),
            pltpu.VMEM((8, half), F32),
            pltpu.VMEM((8, half), F32),
            pltpu.VMEM((8, half), F32),
            pltpu.VMEM((both + 8, half), F32),
            pltpu.VMEM((4, both, half), BF16),
            pltpu.VMEM((4, 2, rows, half), BF16),
            pltpu.VMEM((2, tp, rows, feats), BF16),
            pltpu.VMEM((2, tp, rows, feats), BF16),
            pltpu.VMEM((2, rows, width), F32),
            pltpu.VMEM((2,) + ec.shape, BF16),
            dma((7,)), dma((7,)), dma((7,)),
            dma((7, nz - 1)), dma((7, nz - 1)), dma((7, nz - 1)), dma((7, nz - 1)),
            dma((7,)), dma((7,)), dma, dma, dma((3,)), dma((3,)),
            dma((4,)), dma((4,)), dma((2, tp)), dma((2, tp)), dma((3,)),
        ],
        compiler_params=pltpu.CompilerParams(
            collective_id=0, has_side_effects=True, vmem_limit_bytes=62 * 1024 * 1024
        ),
    )
    return kernel(
        x, gain.reshape(tp, 1, feats), win, wgate, wc, wx, wb, mconv, mlru,
        ctaps, ltaps, wr, wi, odds.reshape(1, width), pos, init.reshape(1, width), ec, el,
    )


def solution(mesh):
    placed = (
        P("sp", "tp"),
        P(),
        P("sp", "tp"),
        P("sp", "tp"),
        P("sp", "tp"),
        P("sp", "tp"),
        P("sp", "tp"),
        P("sp", "tp"),
        P("sp", "tp"),
        P(None, "tp"),
        P(None, "tp"),
        P("tp", None, None),
        P("tp", None, None),
        P("tp"),
        P("sp"),
        P("sp"),
        P("tp"),
        P("tp", None),
        P("tp", None),
    )
    sizes = (mesh.shape["sp"], mesh.shape["tp"])

    def body(*args):
        heads = args[11].shape[0]
        if heads == 2 and sizes[1] == 4 and sizes[0] % 2 == 0 and sizes[0] >= 4:
            return paired(sizes, *args)
        return local(*args)

    return jax.shard_map(
        body, mesh=mesh, in_specs=placed, out_specs=P("sp", "tp"), check_vma=False
    )
```

```python
import functools

import jax
import jax.numpy as jnp
from jax import lax
from jax.experimental import pallas as pl
from jax.experimental.pallas import tpu as pltpu
from jax.sharding import PartitionSpec as P

scan_switch_exponent = 8.0
norm_eps = 1e-06


def passed_along(value, axis, by):
    peers = lax.axis_size(axis)
    pairs = [(i, i + by) for i in range(peers) if 0 <= i + by < peers]
    return lax.ppermute(value, axis, pairs)


def entering(value, axis, combine, identity):
    peers, place = (lax.axis_size(axis), lax.axis_index(axis))
    everything = jax.tree.map(lambda part: lax.all_gather(part, axis), value)
    start = jax.tree.map(
        lambda part, zero: jnp.broadcast_to(jnp.asarray(zero, part.dtype), part.shape),
        value,
        identity,
    )

    def step(k, before):
        reached = k < place
        new = combine(before, jax.tree.map(lambda part: part[k], everything))
        return jax.tree.map(lambda a, b: jnp.where(reached, a, b), new, before)

    return lax.fori_loop(0, peers, step, start)


def linear_chain(earlier, later):
    return (earlier[0] * later[0], later[0] * earlier[1] + later[1])


def causal_local(previous, values, weights):
    taps = weights.shape[0]
    length = values.shape[0]
    extended = jnp.concatenate([previous, values], axis=0)
    result = extended[0:length] * weights[0].astype(jnp.float32)
    for tap_index in range(1, taps):
        result = result + extended[tap_index : tap_index + length] * weights[tap_index].astype(
            jnp.float32
        )
    return result


def local(
    sequence_activations,
    entry_rescale_vector,
    blender_exit_switch_matrix,
    blender_entry_switch_matrix,
    blender_payload_matrix,
    scan_entry_matrix,
    scan_exit_switch_matrix,
    filter_blend_matrix,
    scan_blend_matrix,
    blender_kernel_coefficients,
    scan_kernel_coefficients,
    scan_switch_blockwise,
    entry_switch_blockwise,
    feature_fade_odds,
    fade_speed_multiplier,
    added_rate_shift,
    initial_hidden_vector,
    filter_exit_matrix,
    scan_exit_matrix,
):
    row_count = sequence_activations.shape[0]
    feature_count = entry_rescale_vector.shape[0]
    pieces = [
        blender_exit_switch_matrix,
        blender_entry_switch_matrix,
        blender_payload_matrix,
        scan_entry_matrix,
        scan_exit_switch_matrix,
        filter_blend_matrix,
        scan_blend_matrix,
    ]
    local_cat = jnp.concatenate(pieces, axis=1)
    whole_weight = lax.all_gather(local_cat, "sp", axis=0, tiled=True)
    piece = lax.all_gather(sequence_activations, "tp", axis=1, tiled=True)
    piece_float = piece.astype(jnp.float32)
    scaled_piece = (piece.astype(jnp.float32) * entry_rescale_vector[None, :]).astype(jnp.bfloat16)
    totals = jnp.dot(scaled_piece, whole_weight, preferred_element_type=jnp.float32)
    squares = jnp.sum(piece_float * piece_float, axis=1)
    inverse = lax.rsqrt(squares / feature_count + norm_eps)
    projected = (totals * inverse[:, None]).astype(jnp.bfloat16)
    outputs = []
    offset = 0
    for weight in pieces:
        outputs.append(projected[:, offset : offset + weight.shape[1]])
        offset = offset + weight.shape[1]
    conv_b, conv_c, conv_x, lru_in, lru_gate, mix_conv, mix_lru = outputs
    short_in = conv_c.astype(jnp.float32) * conv_x.astype(jnp.float32)
    lru_float = lru_in.astype(jnp.float32)
    short_edge = blender_kernel_coefficients.shape[0] - 1
    lru_edge = scan_kernel_coefficients.shape[0] - 1
    prev_short, prev_lru = passed_along(
        (short_in[row_count - short_edge :], lru_float[row_count - lru_edge :]), "sp", 1
    )
    lru_conv = causal_local(prev_lru, lru_float, scan_kernel_coefficients).astype(jnp.bfloat16)
    head_local = scan_switch_blockwise.shape[0]
    head_size = scan_switch_blockwise.shape[1]
    lru_local = lru_conv.shape[1]
    heads = lru_conv.reshape(row_count, head_local, head_size)
    scan_switch_amount = jax.nn.sigmoid(
        jnp.einsum("thi,hij->thj", heads, scan_switch_blockwise, preferred_element_type=jnp.float32)
    ).reshape(row_count, lru_local)
    gate_i = jax.nn.sigmoid(
        jnp.einsum(
            "thi,hij->thj", heads, entry_switch_blockwise, preferred_element_type=jnp.float32
        )
    ).reshape(row_count, lru_local)
    position = lax.axis_index("sp") * row_count + jnp.arange(row_count, dtype=jnp.int32)
    fade_exponent_multiplier = (
        scan_switch_exponent
        * scan_switch_amount
        * jax.nn.log_sigmoid(feature_fade_odds)[None, :]
        * fade_speed_multiplier[:, None]
        + added_rate_shift[:, None]
    )
    decay = jnp.exp(fade_exponent_multiplier)
    scale = jnp.sqrt(-jnp.expm1(2.0 * fade_exponent_multiplier))
    scale = jnp.where((position == 0)[:, None], jnp.float32(1.0), scale)
    drive = scale * gate_i * lru_conv.astype(jnp.float32)
    cum_decay, cum_drive = lax.associative_scan(linear_chain, (decay, drive), axis=0)
    ones_state = jnp.ones((lru_local,), jnp.float32)
    zero_state = jnp.zeros((lru_local,), jnp.float32)
    pref_decay, pref_state = entering(
        (cum_decay[-1], cum_drive[-1]), "sp", linear_chain, (ones_state, zero_state)
    )
    carry_in = pref_decay * initial_hidden_vector + pref_state
    state = cum_drive + cum_decay * carry_in[None, :]
    lru_mix = (state * jax.nn.gelu(lru_gate.astype(jnp.float32), approximate=True)).astype(
        jnp.bfloat16
    )
    conv_mix = (
        conv_b.astype(jnp.float32) * causal_local(prev_short, short_in, blender_kernel_coefficients)
    ).astype(jnp.bfloat16)
    conv_part = jnp.dot(conv_mix, filter_exit_matrix, preferred_element_type=jnp.float32)
    lru_part = jnp.dot(lru_mix, scan_exit_matrix, preferred_element_type=jnp.float32)
    conv_sum, lru_sum = (
        lax.psum_scatter(
            conv_part.astype(jnp.bfloat16), "tp", scatter_dimension=1, tiled=True
        ).astype(jnp.float32),
        lax.psum_scatter(
            lru_part.astype(jnp.bfloat16), "tp", scatter_dimension=1, tiled=True
        ).astype(jnp.float32),
    )
    mixed = (
        jax.nn.sigmoid(mix_conv.astype(jnp.float32)) * conv_sum
        + jax.nn.sigmoid(mix_lru.astype(jnp.float32)) * lru_sum
    )
    return mixed.astype(jnp.bfloat16)


MESH = pl.DeviceIdType.MESH
F32, BF16 = jnp.float32, jnp.bfloat16


def small_log1p(u):
    w = 1.0 + u
    return jnp.where(w == 1.0, u, jnp.log(w) * u / jnp.where(w == 1.0, 1.0, w - 1.0))


def neg_expm1(v):
    near = 1.0 + v * (1.0 / 8.0)
    for n in (7, 6, 5, 4, 3, 2):
        near = 1.0 + v * (1.0 / n) * near
    return jnp.where(v > -0.5, -v * near, 1.0 - jnp.exp(v))


def fused_kernel(
    sizes,
    x_hbm, gain, w0, w1, w2, w3, w4, w5, w6,
    ctaps, ltaps, wr, wi, odds, pos, init, ec_hbm, el_hbm,
    out,
    wbuf, xg, xs, sq, inv, posn, lbuf, abuf, bbuf, cbuf, carry_in, carry_out, sbuf,
    mix, got, parts, rbuf, sums, ebuf,
    wl, wx_s, wx_r, zr_s, zr_r, zl_s, zl_r, xg_s, xg_r, po_s, po_r, ed_s, ed_r,
    xe_s, xe_r, rs_s, rs_r, loc, fi_s, fi_r,
):
    sp, tp = sizes
    nz = sp // 2
    s, t = lax.axis_index("sp"), lax.axis_index("tp")
    z, x = s // 2, lax.rem(s, 2)
    xo = 1 - x
    half = wbuf.shape[3]
    rows = x_hbm.shape[0]
    krows = w0.shape[0]
    feats = x_hbm.shape[1]
    both = 2 * rows
    tile = half
    segs = 8
    seg = both // segs
    weights = (w0, w1, w2, w3, w4, w5, w6)
    last = len(weights) - 1
    chunks = [(i, 0, half) for i in range(last)]
    chunks += [(last, 0, half // 2), (last, half // 2, half // 2)]
    count = len(chunks)
    early = 3
    xn = (s + 1 - 2 * x, t)
    core = t + 1 - 2 * lax.rem(t, 2)
    ty = lax.rem(t + 2, tp)
    tyc = lax.rem(core + 2, tp)
    has_l, has_r = z > 0, z < nz - 1
    left, right = (s - 2, t), (s + 2, t)

    def remote(src, dst, ss, rs, dev):
        return pltpu.make_async_remote_copy(
            src_ref=src, dst_ref=dst, send_sem=ss, recv_sem=rs, device_id=dev, device_id_type=MESH
        )

    bar = pltpu.get_barrier_semaphore()
    pl.semaphore_signal(bar, inc=1, device_id=xn, device_id_type=MESH)
    for j in range(1, tp):
        pl.semaphore_signal(bar, inc=1, device_id=(s, lax.rem(t + j, tp)), device_id_type=MESH)

    @pl.when(has_l)
    def _():
        pl.semaphore_signal(bar, inc=1, device_id=left, device_id_type=MESH)

    @pl.when(has_r)
    def _():
        pl.semaphore_signal(bar, inc=1, device_id=right, device_id_type=MESH)

    own_cols = pl.ds(pl.multiple_of(x * half, half), half)

    def weight_cols(p, which):
        i, off, w = chunks[p]
        return weights[i].at[:, pl.ds(pl.multiple_of(which * half + off, half // 2), w)]

    def block(p, zz, xx):
        i, off, w = chunks[p]
        return wbuf.at[i, zz, xx, :, pl.ds(off, w)]

    def line(p, zz):
        i, off, w = chunks[p]
        return wbuf.at[i, zz, :, :, pl.ds(off, w)]

    def own_half(p):
        return pltpu.make_async_copy(weight_cols(p, x), block(p, z, x), wl.at[p])

    def swap_half(p):
        return remote(weight_cols(p, xo), block(p, z, x), wx_s.at[p], wx_r.at[p], xn)

    def swap_half_in(p):
        return remote(weight_cols(p, xo), block(p, z, xo), wx_s.at[p], wx_r.at[p], xn)

    x_in = pltpu.make_async_copy(x_hbm, xg.at[x, t], loc.at[2])
    exits = (
        pltpu.make_async_copy(el_hbm, ebuf.at[0], loc.at[0]),
        pltpu.make_async_copy(ec_hbm, ebuf.at[1], loc.at[1]),
    )
    x_in.start()
    for p in range(count):
        own_half(p).start()
    pl.semaphore_wait(bar, tp + jnp.where(has_l, 1, 0) + jnp.where(has_r, 1, 0))

    for p in range(early):
        swap_half(p).start()
    x_moves = {
        0: lambda: remote(x_hbm, xg.at[x, t], xg_s.at[0], xg_r.at[0], xn),
        1: lambda: remote(x_hbm, xg.at[x, t], xg_s.at[1], xg_r.at[1], (s, ty)),
        2: lambda: remote(x_hbm, xg.at[x, t], xg_s.at[2], xg_r.at[2], (s, core)),
        3: lambda: remote(xg.at[xo, t], xg.at[xo, t], xg_s.at[3], xg_r.at[3], (s, ty)),
        4: lambda: remote(xg.at[xo, t], xg.at[xo, t], xg_s.at[4], xg_r.at[4], (s, core)),
        5: lambda: remote(xg.at[x, ty], xg.at[x, ty], xg_s.at[5], xg_r.at[5], (s, core)),
        6: lambda: remote(xg.at[xo, ty], xg.at[xo, ty], xg_s.at[6], xg_r.at[6], (s, core)),
    }
    x_slots = {
        0: (xo, t), 1: (x, ty), 2: (x, core), 3: (xo, ty),
        4: (xo, core), 5: (x, tyc), 6: (xo, tyc),
    }

    def x_arrive(k):
        a, b = x_slots[k]
        remote(xg.at[a, b], xg.at[a, b], xg_s.at[k], xg_r.at[k], (s, core)).wait_recv()

    for k in (0, 1, 2):
        x_moves[k]().start()
    pos_out = remote(pos, posn.at[x], po_s, po_r, xn)
    pos_out.start()
    for p in range(early, count):
        swap_half(p).start()
    for e in exits:
        e.start()

    def z_right(p, d, part=None):
        if part is not None:
            ref = block(p, z, part)
            return remote(ref, ref, fi_s.at[0], fi_r.at[0], right)
        ref = block(p, z, x) if (p, d) == (0, 0) else line(p, z - d)
        return remote(ref, ref, zr_s.at[p, d], zr_r.at[p, d], right)

    def z_left(p, d, part=None):
        if part is not None:
            ref = block(p, z, part)
            return remote(ref, ref, fi_s.at[1], fi_r.at[1], left)
        ref = block(p, z, x) if (p, d) == (0, 0) else line(p, z + d)
        return remote(ref, ref, zl_s.at[p, d], zl_r.at[p, d], left)

    def from_left(p, d):
        ref = block(p, z - 1, x) if (p, d) == (0, 0) else line(p, z - 1 - d)
        remote(ref, ref, zr_s.at[p, d], zr_r.at[p, d], right).wait_recv()
        if (p, d) == (0, 0):
            ref = block(p, z - 1, xo)
            remote(ref, ref, fi_s.at[0], fi_r.at[0], right).wait_recv()

    def from_right(p, d):
        ref = block(p, z + 1, x) if (p, d) == (0, 0) else line(p, z + 1 + d)
        remote(ref, ref, zl_s.at[p, d], zl_r.at[p, d], left).wait_recv()
        if (p, d) == (0, 0):
            ref = block(p, z + 1, xo)
            remote(ref, ref, fi_s.at[1], fi_r.at[1], left).wait_recv()

    def issue_own(p):
        if p >= count:
            return
        own_half(p).wait()
        if p > 0:
            swap_half_in(p).wait_recv()

        @pl.when(has_r)
        def _():
            z_right(p, 0).start()

        @pl.when(has_l)
        def _():
            z_left(p, 0).start()

        if p > 0:
            return
        swap_half_in(p).wait_recv()

        @pl.when(has_r)
        def _():
            z_right(p, 0, xo).start()

        @pl.when(has_l)
        def _():
            z_left(p, 0, xo).start()

    relayed = set()

    def relay(p, d):
        if p >= count or d >= nz - 1 or (p, d) in relayed:
            return
        relayed.add((p, d))

        @pl.when(z - 1 - d >= 0)
        def _():
            from_left(p, d)
            if d + 1 < nz - 1:
                @pl.when(has_r)
                def _():
                    z_right(p, d + 1).start()

        @pl.when(z + 1 + d < nz)
        def _():
            from_right(p, d)
            if d + 1 < nz - 1:
                @pl.when(has_l)
                def _():
                    z_left(p, d + 1).start()

    def scale_block(a, b):
        for i in range(rows // tile):
            piece = xg[a, b, pl.ds(i * tile, tile), :].astype(F32)
            at = pl.ds(pl.multiple_of(a * rows + i * tile, tile), tile)
            xs[b, at, :] = (piece * gain[b]).astype(BF16)
            square = piece * piece
            total = square[:, 0:128]
            for c in range(1, feats // 128):
                total = total + square[:, c * 128 : (c + 1) * 128]
            sq[at, :] += total

    issue_own(0)
    issue_own(1)
    issue_own(2)
    sq[...] = jnp.zeros_like(sq)
    x_in.wait()
    scale_block(x, t)
    relay(0, 0)
    x_arrive(2)
    scale_block(x, core)
    x_arrive(1)
    x_moves[5]().start()
    scale_block(x, ty)
    relay(0, 1)
    x_arrive(0)
    x_moves[3]().start()
    x_moves[4]().start()
    scale_block(xo, t)
    x_arrive(5)
    scale_block(x, tyc)
    relay(0, 2)
    relay(1, 0)
    x_arrive(4)
    scale_block(xo, core)
    relay(1, 1)
    issue_own(3)
    x_arrive(3)
    x_moves[6]().start()
    scale_block(xo, ty)
    x_arrive(6)
    scale_block(xo, tyc)
    total = jnp.sum(sq[...], axis=1, keepdims=True)
    inv[...] = jnp.broadcast_to(lax.rsqrt(total / (feats * tp) + norm_eps), inv.shape)
    posn[x] = pos[...]
    remote(pos, posn.at[xo], po_s, po_r, xn).wait_recv()

    def project(p, use):
        per = krows * 2
        n, off, width = chunks[p]

        def step(i, _):
            at = pl.ds(pl.multiple_of(i * tile, tile), tile)
            acc = None
            for b in range(tp):
                lhs = xs[b, at, :]
                for zz in range(b * feats // per, (b + 1) * feats // per):
                    for xx in range(2):
                        k0 = zz * per + xx * krows - b * feats
                        term = jnp.dot(
                            lhs[:, k0 : k0 + krows],
                            wbuf[n, zz, xx, :, off : off + width],
                            preferred_element_type=F32,
                        )
                        acc = term if acc is None else acc + term
            wide = inv[at, :]
            scale = jnp.concatenate([wide] * (width // 128), axis=1)
            use(at, i, (acc * scale).astype(BF16))
            return 0

        lax.fori_loop(0, both // tile, step, 0)

    def edge(buf, k):
        return remote(buf.at[pl.ds(both, 8)], buf.at[pl.ds(0, 8)], ed_s.at[k], ed_r.at[k], right)

    def edge_send(buf, k):
        @pl.when(has_r)
        def _():
            edge(buf, k).start()

        @pl.when(z == 0)
        def _():
            buf[0:8, :] = jnp.zeros((8, half), F32)

    def edge_wait(buf, k):
        @pl.when(has_l)
        def _():
            edge(buf, k).wait_recv()

    def carry_copy():
        return remote(carry_out, carry_in, ed_s.at[2], ed_r.at[2], right)

    def swap_part(k):
        if k < 3:
            return k, slice(0, half)
        return 3, slice((k - 3) * (half // 2), (k - 2) * (half // 2))

    def swap(k):
        at = pl.ds(pl.multiple_of(xo * rows, rows), rows)
        m, cols = swap_part(k)
        return remote(
            mix.at[m, at, cols], got.at[m, x, :, cols], xe_s.at[k], xe_r.at[k], xn
        )

    def swap_start(k):
        swap(k).start()
        m, cols = swap_part(k)
        at = pl.ds(pl.multiple_of(x * rows, rows), rows)
        got[m, x, :, cols] = mix[m, at, cols]

    def swap_wait(k):
        m, cols = swap_part(k)
        remote(
            mix.at[m, pl.ds(0, rows), cols], got.at[m, xo, :, cols], xe_s.at[k], xe_r.at[k], xn
        ).wait_recv()

    homes = (t, core, ty, tyc)

    def exchange(e, j):
        peer = homes[2] if j == 2 else homes[1]
        return remote(parts.at[e, j], rbuf.at[e, j], rs_s.at[e, j], rs_r.at[e, j], (s, peer))

    def exit_matmul(e):
        exits[e].wait()
        for j in (3, 1, 0, 2):
            cols = pl.ds(pl.multiple_of(homes[j] * feats, feats), feats)
            if j == 2:
                exchange(e, 3).wait_recv()

            def step(i, _):
                at = pl.ds(pl.multiple_of(i * tile, tile), tile)
                acc = jnp.dot(
                    got[e, 0, at, :], ebuf[e, 0:half, cols], preferred_element_type=F32
                ) + jnp.dot(
                    got[e, 1, at, :], ebuf[e, half : 2 * half, cols], preferred_element_type=F32
                )
                if j == 2:
                    acc = acc + rbuf[e, 3, at, :].astype(F32)
                parts[e, j, at, :] = acc.astype(BF16)
                return 0

            lax.fori_loop(0, rows // tile, step, 0)
            if j > 0:
                exchange(e, j).start()

    def exit_sum(e):
        total = parts[e, 0].astype(F32)
        for j in (1, 2):
            exchange(e, j).wait_recv()
            total = total + rbuf[e, j].astype(F32)
        sums[e] = total

    def finish_stage(p):
        for d in range(nz - 1):
            relay(p, d)
        issue_own(p + 3)


    def keep_lru(at, i, value):
        lbuf[pl.ds(pl.multiple_of(8 + i * tile, 8), tile), :] = value.astype(F32)

    project(0, keep_lru)
    edge_send(lbuf, 0)
    relay(1, 1)
    edge_wait(lbuf, 0)
    rate = -scan_switch_exponent * small_log1p(jnp.exp(-odds[:, own_cols]))
    lanes = ltaps[:, own_cols].astype(F32)
    taps = ltaps.shape[0]
    for i in range(both // tile):
        conv = None
        for k in range(taps):
            term = lbuf[pl.ds(8 - (taps - 1) + k + i * tile, tile), :] * lanes[k : k + 1]
            conv = term if conv is None else conv + term
        conv = conv.astype(BF16)
        gate_r = jax.nn.sigmoid(jnp.dot(conv, wr[x], preferred_element_type=F32))
        gate_i = jax.nn.sigmoid(jnp.dot(conv, wi[x], preferred_element_type=F32))
        first = (i * tile) // rows
        local_at = i * tile - first * rows
        turned = posn[first].T
        speed = turned[local_at : local_at + tile, 0:1]
        shift = turned[local_at : local_at + tile, 1:2]
        log_a = gate_r * rate * speed + shift
        gain_in = jnp.sqrt(neg_expm1(2.0 * log_a))
        if i == 0:
            row = lax.broadcasted_iota(jnp.int32, gain_in.shape, 0) + z * both
            gain_in = jnp.where(row == 0, 1.0, gain_in)
        decay = jnp.exp(log_a)
        drive = gain_in * gate_i * conv.astype(F32)
        for c in range(half // 128):
            cols = slice(c * 128, (c + 1) * 128)
            abuf[c, pl.ds(i * tile, tile), :] = decay[:, cols]
            bbuf[c, pl.ds(i * tile, tile), :] = drive[:, cols]

    lanes_n = half // 128

    def scan_step(i, held):
        cum, state = list(held[:lanes_n]), list(held[lanes_n:])
        at = pl.ds(i, segs, stride=seg)
        for c in range(lanes_n):
            a = abuf[c, at, :]
            state[c] = a * state[c] + bbuf[c, at, :]
            cum[c] = cum[c] * a
            abuf[c, at, :] = cum[c]
            bbuf[c, at, :] = state[c]
        return tuple(cum) + tuple(state)

    ends = lax.fori_loop(
        0, seg, scan_step,
        tuple(jnp.ones((segs, 128), F32) for _ in range(lanes_n))
        + tuple(jnp.zeros((segs, 128), F32) for _ in range(lanes_n)),
        unroll=8,
    )
    end_a = jnp.concatenate(ends[:lanes_n], axis=1)
    end_b = jnp.concatenate(ends[lanes_n:], axis=1)

    @pl.when(z == 0)
    def _():
        carry_in[...] = jnp.broadcast_to(init[:, own_cols], carry_in.shape)

    finish_stage(1)

    @pl.when(has_l)
    def _():
        carry_copy().wait_recv()

    carry = carry_in[0:1, :]
    for j in range(segs):
        cbuf[j : j + 1, :] = carry
        carry = end_b[j : j + 1] + end_a[j : j + 1] * carry
    carry_out[...] = jnp.broadcast_to(carry, carry_out.shape)

    @pl.when(has_r)
    def _():
        carry_copy().start()

    def keep_gate(at, i, value):
        gate = jax.nn.gelu(value.astype(F32), approximate=True)
        pieces = []
        for j in range(tile // seg):
            here = pl.ds(pl.multiple_of(i * tile + j * seg, seg), seg)
            c = cbuf[pl.ds(i * (tile // seg) + j, 1), :]
            pieces.append(
                jnp.concatenate(
                    [
                        bbuf[n, here, :] + abuf[n, here, :] * c[:, n * 128 : (n + 1) * 128]
                        for n in range(half // 128)
                    ],
                    axis=1,
                )
            )
        mix[0, at, :] = (jnp.concatenate(pieces, axis=0) * gate).astype(BF16)

    project(1, keep_gate)
    swap_start(0)
    finish_stage(2)

    def keep_c(at, i, value):
        sbuf[pl.ds(pl.multiple_of(8 + i * tile, 8), tile), :] = value.astype(F32)

    project(2, keep_c)
    swap_wait(0)
    exit_matmul(0)
    finish_stage(3)

    def keep_cx(at, i, value):
        here = pl.ds(pl.multiple_of(8 + i * tile, 8), tile)
        sbuf[here, :] = sbuf[here, :] * value.astype(F32)

    project(3, keep_cx)
    edge_send(sbuf, 1)
    finish_stage(4)

    def keep_b(at, i, value):
        lbuf[pl.ds(pl.multiple_of(8 + i * tile, 8), tile), :] = value.astype(F32)

    @pl.when(has_r)
    def _():
        edge(lbuf, 0).wait_send()

    project(4, keep_b)
    edge_wait(sbuf, 1)
    clanes = ctaps[:, own_cols].astype(F32)
    ktaps = ctaps.shape[0]
    for i in range(both // tile):
        conv = None
        for k in range(ktaps):
            term = sbuf[pl.ds(8 - (ktaps - 1) + k + i * tile, tile), :] * clanes[k : k + 1]
            conv = term if conv is None else conv + term
        mix[1, pl.ds(i * tile, tile), :] = (lbuf[pl.ds(8 + i * tile, tile), :] * conv).astype(BF16)
    swap_start(1)
    swap_wait(1)
    exit_matmul(1)
    for d in range(nz - 1):
        relay(5, d)

    def keep_mix(k):
        m, cols = swap_part(k)

        def use(at, i, value):
            mix[m, at, cols] = value
        return use

    def merge(part):
        for xx in range(2):
            here = slice(part * (half // 2), (part + 1) * (half // 2))
            start = xx * half + part * (half // 2)
            cols = slice(start, start + half // 2)
            out[:, cols] = (
                jax.nn.sigmoid(got[2, xx, :, here].astype(F32)) * sums[1, :, cols]
                + jax.nn.sigmoid(got[3, xx, :, here].astype(F32)) * sums[0, :, cols]
            ).astype(BF16)

    project(5, keep_mix(2))
    swap_start(2)
    exit_sum(0)
    for p in (6, 7):
        for d in range(nz - 1):
            relay(p, d)
        project(p, keep_mix(p - 3))
        swap_start(p - 3)
    exit_sum(1)
    swap_wait(2)
    for part in range(2):
        swap_wait(3 + part)
        merge(part)

    pos_out.wait_send()
    for p in range(count):
        swap_half(p).wait_send()
        if p == 0:
            @pl.when(has_r)
            def _():
                z_right(0, 0, xo).wait_send()

            @pl.when(has_l)
            def _():
                z_left(0, 0, xo).wait_send()

        for d in range(nz - 1):
            @pl.when(has_r & (z - d >= 0))
            def _():
                z_right(p, d).wait_send()

            @pl.when(has_l & (z + d < nz))
            def _():
                z_left(p, d).wait_send()
    for k in x_moves:
        x_moves[k]().wait_send()

    @pl.when(has_r)
    def _():
        edge(sbuf, 1).wait_send()
        carry_copy().wait_send()

    for k in range(5):
        swap(k).wait_send()
    for e in range(2):
        for j in range(1, tp):
            exchange(e, j).wait_send()


def paired(sizes, *args):
    (
        x, gain, wb, wc, wx, win, wgate, mconv, mlru, ctaps, ltaps, wr, wi,
        odds, speed, shift, init, ec, el,
    ) = args
    sp, tp = sizes
    nz = sp // 2
    rows, feats = x.shape
    krows, width = wb.shape
    half = width // 2
    both = 2 * rows
    pos = jnp.concatenate(
        [speed[None], shift[None], jnp.zeros((6, rows), F32)], axis=0
    )
    vmem = pl.BlockSpec(memory_space=pltpu.VMEM)
    anys = pl.BlockSpec(memory_space=pl.ANY)
    dma = pltpu.SemaphoreType.DMA
    kernel = pl.pallas_call(
        functools.partial(fused_kernel, sizes),
        out_shape=jax.ShapeDtypeStruct((rows, width), BF16),
        in_specs=[anys, vmem] + [anys] * 7 + [vmem] * 7 + [anys] * 2,
        out_specs=vmem,
        scratch_shapes=[
            pltpu.VMEM((7, nz, 2, krows, half), BF16),
            pltpu.VMEM((2, tp, rows, feats), BF16),
            pltpu.VMEM((tp, both, feats), BF16),
            pltpu.VMEM((both, 128), F32),
            pltpu.VMEM((both, 128), F32),
            pltpu.VMEM((2, 8, rows), F32),
            pltpu.VMEM((both + 8, half), F32),
            pltpu.VMEM((half // 128, both, 128), F32),
            pltpu.VMEM((half // 128, both, 128), F32),
            pltpu.VMEM((8, half), F32),
            pltpu.VMEM((8, half), F32),
            pltpu.VMEM((8, half), F32),
            pltpu.VMEM((both + 8, half), F32),
            pltpu.VMEM((4, both, half), BF16),
            pltpu.VMEM((4, 2, rows, half), BF16),
            pltpu.VMEM((2, tp, rows, feats), BF16),
            pltpu.VMEM((2, tp, rows, feats), BF16),
            pltpu.VMEM((2, rows, width), F32),
            pltpu.VMEM((2,) + ec.shape, BF16),
            dma((8,)), dma((8,)), dma((8,)),
            dma((8, nz - 1)), dma((8, nz - 1)), dma((8, nz - 1)), dma((8, nz - 1)),
            dma((7,)), dma((7,)), dma, dma, dma((3,)), dma((3,)),
            dma((5,)), dma((5,)), dma((2, tp)), dma((2, tp)), dma((3,)), dma((2,)), dma((2,)),
        ],
        compiler_params=pltpu.CompilerParams(
            collective_id=0, has_side_effects=True, vmem_limit_bytes=62 * 1024 * 1024
        ),
    )
    return kernel(
        x, gain.reshape(tp, 1, feats), win, wgate, wc, wx, wb, mconv, mlru,
        ctaps, ltaps, wr, wi, odds.reshape(1, width), pos, init.reshape(1, width), ec, el,
    )


def solution(mesh):
    placed = (
        P("sp", "tp"),
        P(),
        P("sp", "tp"),
        P("sp", "tp"),
        P("sp", "tp"),
        P("sp", "tp"),
        P("sp", "tp"),
        P("sp", "tp"),
        P("sp", "tp"),
        P(None, "tp"),
        P(None, "tp"),
        P("tp", None, None),
        P("tp", None, None),
        P("tp"),
        P("sp"),
        P("sp"),
        P("tp"),
        P("tp", None),
        P("tp", None),
    )
    sizes = (mesh.shape["sp"], mesh.shape["tp"])

    def body(*args):
        heads = args[11].shape[0]
        if heads == 2 and sizes[1] == 4 and sizes[0] % 2 == 0 and sizes[0] >= 4:
            return paired(sizes, *args)
        return local(*args)

    return jax.shard_map(
        body, mesh=mesh, in_specs=placed, out_specs=P("sp", "tp"), check_vma=False
    )
```
